32 devices in a mesh: sp: 2 (over x), dp: 16 (over z, y, core).
Axes of the slice: x: 2, y: 2, z: 4, core: 2. Of those that a mesh axis runs over, the one named last changes fastest.
Arguments:
- hidden_in: bfloat16 [1024, 2048], P('sp'), may hold values from -6 to 6
- content_weight: bfloat16 [2048, 2048], P('sp', 'dp'), may hold values from -0.125 to 0.125
- gating_weight: bfloat16 [2048, 2048], P('sp', 'dp'), may hold values from -2 to 2
- norm_gain: float32 [2048], P('dp'), may hold values from 0.1 to 1.9
- mixing_weight: bfloat16 [16, 128, 128], P('dp'), may hold values from -0.5 to 0.5
- mixing_bias: float32 [16, 128], P('dp'), may hold values from 0.1 to 1.9
- out_grad: bfloat16 [1024, 2048], P('sp', 'dp'), may hold values from -13 to 13
Outputs:
- input_grad: bfloat16 [1024, 2048], P('sp', 'dp')
- content_grad: float32 [2048, 2048], P('sp', 'dp')
- gating_grad: float32 [2048, 2048], P('sp', 'dp')
- mixing_grad: float32 [16, 128, 128], P('dp')
The draws below stay inside these ranges and needn't reach their ends.
All inputs are finite; a program needn't handle non-finite values.
Results may differ from the reference program's by a relative error of at most 0.019.
Values may be sent and summed in bfloat16 or wider, within the bound.
A program may use at most 64 MiB of HBM per device.

```python
import math
import jax
import jax.numpy as jnp
from jax import lax

D = 2048
G = 16
GROUP_DIM = 128
BLOCK = 128
F = 2048
TOKENS = 1024
N_DP = 16


def column_scales(key):
    group_of = (jnp.arange(F) // GROUP_DIM).astype(jnp.float32)
    rising = group_of / (G - 1)
    jitter = jax.random.uniform(key, (F,), jnp.float32)
    exponent = 0.5 * rising + 0.5 * jitter
    return 10.0 ** (exponent - 0.5)


def draw_gating_weight(key, part):
    entries = jax.random.truncated_normal(jax.random.fold_in(key, 11), -4.0, 4.0, (D, F), jnp.float32)
    scales = column_scales(jax.random.fold_in(key, 12))
    return (entries * scales[None, :] * D ** (-0.5)).astype(jnp.bfloat16)


def draw_out_grad(key, part):
    entries = jax.random.truncated_normal(jax.random.fold_in(key, 21), -4.0, 4.0, (TOKENS, F), jnp.float32)
    scales = column_scales(jax.random.fold_in(key, 22))
    return (entries * scales[None, :]).astype(jnp.bfloat16)


def level_of(stream_key, extent, cuts, low, top_value):
    gain = 1.0
    for axis_at, blocks in cuts:
        draws = jax.random.uniform(jax.random.fold_in(jax.random.fold_in(stream_key, 6), axis_at), (blocks,), jnp.float32, low / len(cuts), top_value / len(cuts))
        gain = gain * jnp.repeat(jnp.exp(draws), extent[axis_at] // blocks).reshape((-1,) + (1,) * (len(extent) - 1 - axis_at))
    return gain


def bell_draw(own_key, extent, scale, limit, pieces=(), kind=jnp.bfloat16):
    result = jax.random.normal(own_key, extent, jnp.float32) * scale
    if len(pieces) > 0:
        result = level_of(own_key, extent, pieces, -0.22, 0.18) * result
    return jnp.clip(result, min=-limit, max=limit).astype(kind)


def setup_inputs(seed: int = 0) -> dict:
    seeds = jax.random.split(jax.random.key(seed), 8)
    hidden_in = bell_draw(seeds[0], (TOKENS, D), 1.0, 6.0, ((0, 2),))
    content_weight = bell_draw(seeds[1], (D, F), D ** -0.5, 0.125, ((0, 2), (1, 16)))
    gating_weight = draw_gating_weight(jax.random.fold_in(seeds[7], 71), 0)
    norm_gain = jnp.clip(1.0 + 0.18 * jax.random.normal(seeds[3], (F,), jnp.float32), 0.1, 1.9)
    mixing_weight = bell_draw(seeds[4], (G, BLOCK, BLOCK), BLOCK ** -0.5, 0.5, ((0, 16),))
    mixing_bias = jnp.clip(1.0 + 0.18 * jax.random.normal(seeds[5], (G, BLOCK), jnp.float32), 0.1, 1.9)
    out_grad = draw_out_grad(jax.random.fold_in(seeds[7], 71), 0)
    return dict(hidden_in=hidden_in, content_weight=content_weight, gating_weight=gating_weight, norm_gain=norm_gain, mixing_weight=mixing_weight, mixing_bias=mixing_bias, out_grad=out_grad)


norm_eps = 1e-05

def gelu_slope(values):
    cumulative = 0.5 * (1.0 + lax.erf(values * (1.0 / math.sqrt(2.0))))
    density = jnp.exp(-0.5 * values * values) * (1.0 / math.sqrt(2.0 * math.pi))
    return cumulative + values * density

def stored(values):
    return lax.optimization_barrier(values.astype(jnp.bfloat16))

def causal_table(weights):
    row_ids = lax.broadcasted_iota(jnp.int32, (BLOCK, BLOCK), 0)
    col_ids = lax.broadcasted_iota(jnp.int32, (BLOCK, BLOCK), 1)
    keeper = (col_ids <= row_ids)[None]
    return (jnp.where(keeper, weights, jnp.zeros_like(weights)), keeper)

def reference(hidden_in, content_weight, gating_weight, norm_gain, mixing_weight, mixing_bias, out_grad):
    tokens = hidden_in.shape[0]
    width = content_weight.shape[1]
    groups = width // GROUP_DIM
    blocks = tokens // BLOCK
    grad_scale = 1.0 / math.sqrt(tokens)
    pre_content = stored(jnp.dot(hidden_in, content_weight, preferred_element_type=jnp.float32)).astype(jnp.float32)
    pre_gating = stored(jnp.dot(hidden_in, gating_weight, preferred_element_type=jnp.float32)).astype(jnp.float32)
    content = jax.nn.gelu(pre_content, approximate=False)
    gating = jax.nn.gelu(pre_gating, approximate=False)
    row_mean = lax.optimization_barrier(jnp.mean(gating, axis=1, keepdims=True))
    row_var = lax.optimization_barrier(jnp.mean(gating * gating, axis=1, keepdims=True)) - row_mean * row_mean
    inv_std = lax.rsqrt(row_var + norm_eps)
    centred = (gating - row_mean) * inv_std
    normed = (centred * norm_gain[None, :]).astype(jnp.bfloat16)
    spatial, keeper = causal_table(mixing_weight)
    spatial_wide = spatial.astype(jnp.float32)
    normed_blocks = normed.astype(jnp.float32).reshape(blocks, BLOCK, groups, GROUP_DIM)
    mixed = jnp.einsum('gts,bsgc->btgc', spatial_wide, normed_blocks)
    mixed = mixed + jnp.transpose(mixing_bias)[None, :, :, None]
    mixed = mixed.reshape(tokens, width)
    grad_wide = out_grad.astype(jnp.float32)
    content_pre_grad = (grad_wide * mixed * gelu_slope(pre_content)).astype(jnp.bfloat16)
    mixed_grad = (grad_wide * content).astype(jnp.bfloat16)
    mixed_blocks = mixed_grad.astype(jnp.float32).reshape(blocks, BLOCK, groups, GROUP_DIM)
    mixing_grad = jnp.where(keeper, jnp.einsum('btgc,bsgc->gts', mixed_blocks, normed_blocks), 0.0) * grad_scale
    normed_grad = jnp.einsum('gts,btgc->bsgc', spatial_wide, mixed_blocks).reshape(tokens, width)
    centred_grad = normed_grad * norm_gain[None, :]
    first_moment = lax.optimization_barrier(jnp.mean(centred_grad, axis=1, keepdims=True))
    second_moment = lax.optimization_barrier(jnp.mean(centred_grad * centred, axis=1, keepdims=True))
    gating_back = inv_std * (centred_grad - first_moment - centred * second_moment)
    gating_pre_grad = (gating_back * gelu_slope(pre_gating)).astype(jnp.bfloat16)
    shard_cols = width // N_DP
    dims = (((1,), (1,)), ((), ()))

    def add_shard(running, shard_index):
        col_start = shard_index * shard_cols
        part_content = lax.dynamic_slice_in_dim(content_pre_grad, col_start, shard_cols, 1)
        part_gating = lax.dynamic_slice_in_dim(gating_pre_grad, col_start, shard_cols, 1)
        weight_content = lax.dynamic_slice_in_dim(content_weight, col_start, shard_cols, 1)
        weight_gating = lax.dynamic_slice_in_dim(gating_weight, col_start, shard_cols, 1)
        term = lax.dot_general(part_content, weight_content, dims, preferred_element_type=jnp.float32)
        term = term + lax.dot_general(part_gating, weight_gating, dims, preferred_element_type=jnp.float32)
        return (running + stored(term).astype(jnp.float32), None)
    input_sum, unused = lax.scan(add_shard, jnp.zeros((tokens, D), jnp.float32), jnp.arange(N_DP, dtype=jnp.int32))
    token_dims = (((0,), (0,)), ((), ()))
    content_grad = lax.dot_general(hidden_in, content_pre_grad, token_dims, preferred_element_type=jnp.float32) * grad_scale
    gating_grad = lax.dot_general(hidden_in, gating_pre_grad, token_dims, preferred_element_type=jnp.float32) * grad_scale
    return (input_sum.astype(jnp.bfloat16), content_grad, gating_grad, mixing_grad)
```

```python
import functools
import math

import jax
import jax.numpy as jnp
from jax import lax
from jax.experimental import pallas as pl
from jax.experimental.pallas import tpu as pltpu
from jax.sharding import PartitionSpec as P

GROUP_DIM = 128
BLOCK = 128


norm_eps = 1e-05


def gelu_slope(values):
    cumulative = 0.5 * (1.0 + lax.erf(values * (1.0 / math.sqrt(2.0))))
    density = jnp.exp(-0.5 * values * values) * (1.0 / math.sqrt(2.0 * math.pi))
    return cumulative + values * density


def causal_table(weights):
    row_ids = lax.broadcasted_iota(jnp.int32, (BLOCK, BLOCK), 0)
    col_ids = lax.broadcasted_iota(jnp.int32, (BLOCK, BLOCK), 1)
    keeper = (col_ids <= row_ids)[None]
    return (jnp.where(keeper, weights, jnp.zeros_like(weights)), keeper)


def hidden_term(hidden_in, grads):
    return lax.dot_general(
        hidden_in, grads, (((0,), (0,)), ((), ())), preferred_element_type=jnp.float32
    )


def local(
    hidden_in, content_weight, gating_weight, norm_gain, mixing_weight, mixing_bias, out_grad
):
    tok_rows = hidden_in.shape[0]
    local_width = content_weight.shape[1]
    groups_here = local_width // GROUP_DIM
    blocks = tok_rows // BLOCK
    full_width = local_width * lax.axis_size("dp")
    grad_scale = 1.0 / math.sqrt(tok_rows * lax.axis_size("sp"))
    whole_content, whole_gating = (
        lax.all_gather(content_weight, "sp", axis=0, tiled=True),
        lax.all_gather(gating_weight, "sp", axis=0, tiled=True),
    )
    joined_weight = jnp.concatenate([whole_content, whole_gating], axis=1)
    pre_both = jnp.dot(hidden_in, joined_weight, preferred_element_type=jnp.float32).astype(
        jnp.bfloat16
    )
    pre_content = pre_both[:, :local_width].astype(jnp.float32)
    pre_gating = pre_both[:, local_width:].astype(jnp.float32)
    content = jax.nn.gelu(pre_content, approximate=False)
    gating = jax.nn.gelu(pre_gating, approximate=False)
    spatial, keeper = causal_table(mixing_weight)
    grad_wide = out_grad.astype(jnp.float32)
    mixed_grad = (grad_wide * content).astype(jnp.bfloat16)
    mixed_blocks = mixed_grad.reshape(blocks, BLOCK, groups_here, GROUP_DIM)
    normed_grad = jnp.einsum(
        "gts,btgc->bsgc", spatial, mixed_blocks, preferred_element_type=jnp.float32
    )
    centred_grad = normed_grad.reshape(tok_rows, local_width) * norm_gain[None, :]
    row_sum, row_square, grad_sum, grad_raw = lax.psum(
        (
            jnp.sum(gating, axis=1),
            jnp.sum(gating * gating, axis=1),
            jnp.sum(centred_grad, axis=1),
            jnp.sum(centred_grad * gating, axis=1),
        ),
        "dp",
    )
    row_mean = (row_sum / full_width)[:, None]
    row_var = (row_square / full_width)[:, None] - row_mean * row_mean
    inv_std = lax.rsqrt(row_var + norm_eps)
    centred = (gating - row_mean) * inv_std
    first_moment = (grad_sum / full_width)[:, None]
    second_moment = inv_std * ((grad_raw / full_width)[:, None] - row_mean * first_moment)
    normed = (centred * norm_gain[None, :]).astype(jnp.bfloat16)
    normed_blocks = normed.reshape(blocks, BLOCK, groups_here, GROUP_DIM)
    mixed = jnp.einsum("gts,bsgc->btgc", spatial, normed_blocks, preferred_element_type=jnp.float32)
    mixed = (mixed + jnp.transpose(mixing_bias)[None, :, :, None]).reshape(tok_rows, local_width)
    content_pre_grad = (grad_wide * mixed * gelu_slope(pre_content)).astype(jnp.bfloat16)
    local_mixing = jnp.einsum(
        "btgc,bsgc->gts", mixed_blocks, normed_blocks, preferred_element_type=jnp.float32
    )
    local_mixing = jnp.where(keeper, local_mixing, 0.0)
    mixing_grad = lax.psum(local_mixing.astype(jnp.bfloat16), "sp").astype(jnp.float32) * grad_scale
    gating_back = inv_std * (centred_grad - first_moment - centred * second_moment)
    gating_pre_grad = (gating_back * gelu_slope(pre_gating)).astype(jnp.bfloat16)
    joined_grad = jnp.concatenate([content_pre_grad, gating_pre_grad], axis=1)
    partial_input = lax.dot_general(
        joined_grad, joined_weight, (((1,), (1,)), ((), ())), preferred_element_type=jnp.float32
    )
    input_grad = lax.psum_scatter(
        partial_input.astype(jnp.bfloat16), "dp", scatter_dimension=1, tiled=True
    )
    both_grads = (
        lax.psum_scatter(
            hidden_term(hidden_in, joined_grad).astype(jnp.bfloat16),
            "sp",
            scatter_dimension=0,
            tiled=True,
        ).astype(jnp.float32)
        * grad_scale
    )
    content_grad = both_grads[:, :local_width]
    gating_grad = both_grads[:, local_width:]
    return (input_grad, content_grad, gating_grad, mixing_grad)


def phi_and_slope(values):
    cumulative = 0.5 * (1.0 + lax.erf(values * (1.0 / math.sqrt(2.0))))
    density = jnp.exp(-0.5 * values * values) * (1.0 / math.sqrt(2.0 * math.pi))
    return cumulative, cumulative + values * density


def dot(a, b, ca, cb):
    return lax.dot_general(
        a, b, (((ca,), (cb,)), ((), ())), preferred_element_type=jnp.float32
    )


def fused_kernel(
    n_dp, full_width, grad_scale,
    h_in, wc_in, wg_in, gain_ref, mix_ref, bias_ref, og_in,
    x_out, c_out, g_out, m_out,
    hid, hid_t, wts, og, cg, cg_t, cs, gat, slope_g, mg, joined,
    stat_a, stat_quad, stat_b, stat_z,
    part, r_core, q_send, r_y, z_send, r_z, acc,
    gs, gr, go, ms, mr,
    load_sem, w_send, w_recv, sq_send, sq_recv, sz_send, sz_recv,
    core_send, core_recv, y_send, y_recv, zz_send, zz_recv,
    gx_send, gx_recv, mx_send, mx_recv,
):
    toks = hid.shape[0]
    chunks = toks // BLOCK
    shard = wc_in.shape[0]
    nz = n_dp // 4
    half = toks // 2
    tiles = gs.shape[0]
    tile = gs.shape[1]
    bf16 = jnp.bfloat16
    f32 = jnp.float32

    i = lax.axis_index("sp")
    j = lax.axis_index("dp")
    x_peer = 1 - i
    c = lax.rem(j, 2)
    y = lax.rem(j // 2, 2)
    z = j // 4
    j_core = j + 1 - 2 * c
    j_y = j + 2 - 4 * y
    j_diag = j_core + 2 - 4 * y

    def z_dev(q):
        return lax.rem(z + q, nz) * 4 + y * 2 + c

    def dev(a, b):
        return {"sp": a, "dp": b}

    def remote(src, dst, ssem, rsem, target):
        return pltpu.make_async_remote_copy(
            src_ref=src, dst_ref=dst, send_sem=ssem, recv_sem=rsem,
            device_id=target, device_id_type=pl.DeviceIdType.MESH,
        )

    mine = pl.multiple_of(i * shard, shard)
    theirs = pl.multiple_of(x_peer * shard, shard)
    loads = [
        pltpu.make_async_copy(wc_in, wts.at[pl.ds(mine, shard), pl.ds(0, BLOCK)], load_sem.at[0]),
        pltpu.make_async_copy(h_in, hid, load_sem.at[1]),
        pltpu.make_async_copy(wg_in, wts.at[pl.ds(mine, shard), pl.ds(BLOCK, BLOCK)], load_sem.at[2]),
        pltpu.make_async_copy(og_in, og, load_sem.at[3]),
    ]
    for load in loads:
        load.start()

    barrier = pltpu.get_barrier_semaphore()
    peers = [dev(x_peer, j), dev(i, j_core), dev(i, j_y), dev(i, j_diag)]
    peers += [dev(i, z_dev(q)) for q in range(1, nz)]
    for peer in peers:
        pl.semaphore_signal(barrier, inc=1, device_id=peer, device_id_type=pl.DeviceIdType.MESH)
    pl.semaphore_wait(barrier, len(peers))

    pieces = w_send.shape[0] // 2
    piece = shard // pieces
    w_copies = []
    for which, src in ((0, wc_in), (1, wg_in)):
        for p in range(pieces):
            copy = remote(
                src.at[pl.ds(p * piece, piece), :],
                wts.at[pl.ds(pl.multiple_of(mine + p * piece, piece), piece), pl.ds(which * BLOCK, BLOCK)],
                w_send.at[which * pieces + p], w_recv.at[which * pieces + p],
                dev(x_peer, j),
            )
            copy.start()
            w_copies.append(copy)

    keep = lax.broadcasted_iota(jnp.int32, (BLOCK, BLOCK), 1) <= lax.broadcasted_iota(
        jnp.int32, (BLOCK, BLOCK), 0
    )
    spatial = jnp.where(keep, mix_ref[0].astype(f32), 0.0).astype(bf16)
    gain = gain_ref[...]
    bias = jnp.broadcast_to(bias_ref[...], (BLOCK, BLOCK)).T

    for load in loads:
        load.wait()
    own = dot(hid[:, pl.ds(mine, shard)], wts[pl.ds(mine, shard), :], 1, 0)
    joined_pre = own
    acc_c = go.at[pl.ds(0, toks), pl.ds(0, BLOCK)]
    acc_g = go.at[pl.ds(0, toks), pl.ds(BLOCK, BLOCK)]
    go[pl.ds(0, toks), :] = joined_pre
    for b in range(hid.shape[1] // BLOCK):
        hid_t[pl.ds(b * BLOCK, BLOCK), :] = hid[:, pl.ds(b * BLOCK, BLOCK)].T

    def finish(which, target):
        for p in range(pieces):
            w_copies[which * pieces + p].wait_recv()
            at = pl.multiple_of(theirs + p * piece, piece)
            target[...] += dot(
                hid[:, pl.ds(at, piece)], wts[pl.ds(at, piece), pl.ds(which * BLOCK, BLOCK)], 1, 0
            )

    finish(0, acc_c)
    for k in range(chunks):
        rows = pl.ds(k * BLOCK, BLOCK)
        pre = go[rows, 0:BLOCK].astype(bf16).astype(f32)
        wide = og[rows, :].astype(f32)
        cumulative, slope = phi_and_slope(pre)
        cs[rows, :] = wide * slope
        mixed_grad = (wide * (pre * cumulative)).astype(bf16)
        mg[rows, :] = mixed_grad
        centred_grad = dot(spatial, mixed_grad, 0, 0) * gain
        cg[rows, :] = centred_grad
        cg_t[rows, :] = centred_grad.T

    finish(1, acc_g)
    for k in range(chunks):
        rows = pl.ds(k * BLOCK, BLOCK)
        pre = go[rows, BLOCK:2 * BLOCK].astype(bf16).astype(f32)
        cumulative, slope = phi_and_slope(pre)
        gating = pre * cumulative
        gat[rows, :] = gating
        slope_g[rows, :] = slope
        turned = gating.T
        grad_turned = cg_t[rows, :]
        base = 4 * (k * BLOCK // half)
        cols = pl.ds(k * BLOCK % half, BLOCK)
        for row, table in enumerate((turned, turned * turned, grad_turned, grad_turned * turned)):
            stat_a[base + row:base + row + 1, cols] = jnp.sum(table, axis=0, keepdims=True)

    stat_copies = []
    for s, target in enumerate((j_core, j_y, j_diag)):
        copy = remote(stat_a, stat_quad.at[s], sq_send.at[s], sq_recv.at[s], dev(i, target))
        copy.start()
        stat_copies.append(copy)
    for copy in stat_copies:
        copy.wait()
    stat_b[...] = (stat_a[...] + stat_quad[0]) + (stat_quad[1] + stat_quad[2])
    stat_copies = []
    for q in range(1, nz):
        copy = remote(
            stat_b, stat_z.at[q - 1], sz_send.at[q - 1], sz_recv.at[q - 1], dev(i, z_dev(q))
        )
        copy.start()
        stat_copies.append(copy)
    for copy in stat_copies:
        copy.wait()
    total = stat_b[...]
    for q in range(1, nz):
        total = total + stat_z[q - 1]
    total = total * (1.0 / full_width)

    mixing = jnp.zeros((BLOCK, BLOCK), f32)
    for k in range(chunks):
        rows = pl.ds(k * BLOCK, BLOCK)
        base = 4 * (k * BLOCK // half)
        col = k * BLOCK % half
        part_of = total[base:base + 4, col:col + BLOCK]
        mean = part_of[0:1]
        inv = lax.rsqrt(part_of[1:2] - mean * mean + norm_eps)
        first = part_of[2:3]
        second = inv * (part_of[3:4] - mean * first)

        def spread(row):
            return jnp.broadcast_to(row, (BLOCK, BLOCK)).T

        inv_w = spread(inv)
        centred = (gat[rows, :] - spread(mean)) * inv_w
        normed = (centred * gain).astype(bf16)
        mixed = dot(spatial, normed, 1, 0) + bias
        joined[rows, 0:BLOCK] = (cs[rows, :] * mixed).astype(bf16)
        back = inv_w * (cg[rows, :] - spread(first) - centred * spread(second))
        joined[rows, BLOCK:2 * BLOCK] = (back * slope_g[rows, :]).astype(bf16)
        mixing = mixing + dot(mg[rows, :], normed, 1, 1)
    mixing = jnp.where(keep, mixing, 0.0)

    waits = []

    def input_part(k):
        grads = joined[pl.ds(k * BLOCK, BLOCK), :]
        for zz in range(nz):
            res = dot(grads, wts[pl.ds(zz * 4 * BLOCK, 4 * BLOCK), :], 1, 1).astype(bf16)
            for yy in range(2):
                for cc in range(2):
                    at = (yy * 2 + cc) * BLOCK
                    part[k, cc, yy, zz] = res[:, at:at + BLOCK]
        copy = remote(part.at[k, 1 - c], r_core.at[k], core_send.at[k], core_recv.at[k], dev(i, j_core))
        copy.start()
        waits.append(copy)
        return copy

    def weight_part(t):
        at = pl.multiple_of(theirs + t * tile, tile)
        gs[t] = dot(hid_t[pl.ds(at, tile), :], joined[...], 1, 0).astype(bf16)
        copy = remote(gs.at[t], gr.at[t], gx_send.at[t], gx_recv.at[t], dev(x_peer, j))
        copy.start()
        waits.append(copy)
        return copy

    core_copies, y_copies, z_copies, g_copies = {}, {}, {}, {}

    def second_stage(k):
        core_copies[k].wait_recv()
        q_send[k] = (
            part[k, c, 1 - y].astype(f32) + r_core[k, 1 - y].astype(f32)
        ).astype(bf16)
        copy = remote(q_send.at[k], r_y.at[k], y_send.at[k], y_recv.at[k], dev(i, j_y))
        copy.start()
        waits.append(copy)
        y_copies[k] = copy

    def third_stage(k):
        y_copies[k].wait_recv()
        z_copies[k] = []
        for q in range(1, nz + 1):
            zt = lax.rem(z + q, nz)
            res = (
                part[k, c, y, zt].astype(f32) + r_core[k, y, zt].astype(f32)
            ) + r_y[k, zt].astype(f32)
            if q == nz:
                acc[k] = res
                continue
            z_send[k, q - 1] = res.astype(bf16)
            copy = remote(
                z_send.at[k, q - 1], r_z.at[k, q - 1], zz_send.at[k, q - 1], zz_recv.at[k, q - 1],
                dev(i, z_dev(q)),
            )
            copy.start()
            waits.append(copy)
            z_copies[k].append(copy)

    def last_stage(k):
        res = acc[k]
        for q in range(1, nz):
            z_copies[k][q - 1].wait_recv()
            res = res + r_z[k, q - 1].astype(f32)
        x_out[pl.ds(k * BLOCK, BLOCK), :] = res.astype(bf16)

    for step in range(max(chunks + 2, tiles)):
        if step < chunks:
            core_copies[step] = input_part(step)
        if step < tiles:
            g_copies[step] = weight_part(step)
        if 0 <= step - 1 < chunks:
            second_stage(step - 1)
        if 0 <= step - 2 < chunks:
            third_stage(step - 2)
    ms[...] = mixing.astype(bf16)
    m_copy = remote(ms, mr, mx_send, mx_recv, dev(x_peer, j))
    m_copy.start()
    waits.append(m_copy)
    for t in range(tiles):
        at = pl.multiple_of(mine + t * tile, tile)
        go[pl.ds(t * tile, tile), :] = dot(hid_t[pl.ds(at, tile), :], joined[...], 1, 0)
    for k in range(chunks):
        last_stage(k)
    for t in range(tiles):
        g_copies[t].wait_recv()
        rows = pl.ds(t * tile, tile)
        res = (go[rows, :] + gr[t].astype(f32)) * grad_scale
        c_out[rows, :] = res[:, 0:BLOCK]
        g_out[rows, :] = res[:, BLOCK:2 * BLOCK]
    m_copy.wait_recv()
    m_out[0] = (mixing + mr[...].astype(f32)) * grad_scale
    for copy in w_copies + waits:
        copy.wait_send()


def fused(n_dp, hidden_in, content_weight, gating_weight, norm_gain, mixing_weight, mixing_bias, out_grad):
    toks, depth = hidden_in.shape
    shard, width = content_weight.shape
    chunks = toks // BLOCK
    nz = n_dp // 4
    tile = 256
    tiles = shard // tile
    pieces = 2
    grad_scale = 1.0 / math.sqrt(2 * toks)
    bf16, f32 = jnp.bfloat16, jnp.float32
    vmem = pl.BlockSpec(memory_space=pltpu.VMEM)
    anywhere = pl.BlockSpec(memory_space=pl.ANY)
    dma = pltpu.SemaphoreType.DMA
    V = pltpu.VMEM
    scratch = [
        V((toks, depth), bf16), V((depth, toks), bf16), V((depth, 2 * width), bf16), V((toks, width), bf16),
        V((toks, width), f32), V((toks, width), f32), V((toks, width), f32), V((toks, width), f32),
        V((toks, width), f32), V((toks, width), bf16), V((toks, 2 * width), bf16),
        V((8, toks // 2), f32), V((3, 8, toks // 2), f32), V((8, toks // 2), f32), V((nz - 1, 8, toks // 2), f32),
        V((chunks, 2, 2, nz, BLOCK, width), bf16), V((chunks, 2, nz, BLOCK, width), bf16),
        V((chunks, nz, BLOCK, width), bf16), V((chunks, nz, BLOCK, width), bf16),
        V((chunks, nz - 1, BLOCK, width), bf16), V((chunks, nz - 1, BLOCK, width), bf16), V((chunks, BLOCK, width), f32),
        V((tiles, tile, 2 * width), bf16), V((tiles, tile, 2 * width), bf16), V((shard, 2 * width), f32),
        V((BLOCK, BLOCK), bf16), V((BLOCK, BLOCK), bf16),
        dma((4,)), dma((2 * pieces,)), dma((2 * pieces,)), dma((3,)), dma((3,)), dma((nz - 1,)), dma((nz - 1,)),
        dma((chunks,)), dma((chunks,)), dma((chunks,)), dma((chunks,)), dma((chunks, nz - 1)), dma((chunks, nz - 1)),
        dma((tiles,)), dma((tiles,)), dma, dma,
    ]
    return pl.pallas_call(
        functools.partial(fused_kernel, n_dp, width * n_dp, grad_scale),
        out_shape=(
            jax.ShapeDtypeStruct((toks, width), bf16),
            jax.ShapeDtypeStruct((shard, width), f32),
            jax.ShapeDtypeStruct((shard, width), f32),
            jax.ShapeDtypeStruct(mixing_weight.shape, f32),
        ),
        in_specs=[anywhere, anywhere, anywhere, vmem, vmem, vmem, anywhere],
        out_specs=(vmem,) * 4,
        scratch_shapes=scratch,
        compiler_params=pltpu.CompilerParams(
            collective_id=0, has_side_effects=True, vmem_limit_bytes=40 * 1024 * 1024
        ),
    )(hidden_in, content_weight, gating_weight, norm_gain[None, :], mixing_weight, mixing_bias, out_grad)


def fits(n_sp, n_dp, toks, shard, width):
    paired = n_sp == 2 and n_dp % 4 == 0 and n_dp >= 8
    return paired and width == GROUP_DIM and shard % 512 == 0 and toks % (2 * BLOCK) == 0 and toks <= shard


def solve(*args):
    n_sp, n_dp = lax.axis_size("sp"), lax.axis_size("dp")
    shard, width = args[1].shape
    if fits(n_sp, n_dp, args[0].shape[0], shard, width) and args[0].shape[1] == n_dp * width:
        return fused(n_dp, *args)
    return local(*args)


def solution(mesh):
    in_specs = (
        P("sp", None),
        P("sp", "dp"),
        P("sp", "dp"),
        P("dp"),
        P("dp", None, None),
        P("dp", None),
        P("sp", "dp"),
    )
    out_specs = (P("sp", "dp"), P("sp", "dp"), P("sp", "dp"), P("dp", None, None))
    return jax.shard_map(solve, mesh=mesh, in_specs=in_specs, out_specs=out_specs, check_vma=False)
```

```python
import functools
import math

import jax
import jax.numpy as jnp
from jax import lax
from jax.experimental import pallas as pl
from jax.experimental.pallas import tpu as pltpu
from jax.sharding import PartitionSpec as P

GROUP_DIM = 128
BLOCK = 128


norm_eps = 1e-05


def gelu_slope(values):
    cumulative = 0.5 * (1.0 + lax.erf(values * (1.0 / math.sqrt(2.0))))
    density = jnp.exp(-0.5 * values * values) * (1.0 / math.sqrt(2.0 * math.pi))
    return cumulative + values * density


def causal_table(weights):
    row_ids = lax.broadcasted_iota(jnp.int32, (BLOCK, BLOCK), 0)
    col_ids = lax.broadcasted_iota(jnp.int32, (BLOCK, BLOCK), 1)
    keeper = (col_ids <= row_ids)[None]
    return (jnp.where(keeper, weights, jnp.zeros_like(weights)), keeper)


def hidden_term(hidden_in, grads):
    return lax.dot_general(
        hidden_in, grads, (((0,), (0,)), ((), ())), preferred_element_type=jnp.float32
    )


def local(
    hidden_in, content_weight, gating_weight, norm_gain, mixing_weight, mixing_bias, out_grad
):
    tok_rows = hidden_in.shape[0]
    local_width = content_weight.shape[1]
    groups_here = local_width // GROUP_DIM
    blocks = tok_rows // BLOCK
    full_width = local_width * lax.axis_size("dp")
    grad_scale = 1.0 / math.sqrt(tok_rows * lax.axis_size("sp"))
    whole_content, whole_gating = (
        lax.all_gather(content_weight, "sp", axis=0, tiled=True),
        lax.all_gather(gating_weight, "sp", axis=0, tiled=True),
    )
    joined_weight = jnp.concatenate([whole_content, whole_gating], axis=1)
    pre_both = jnp.dot(hidden_in, joined_weight, preferred_element_type=jnp.float32).astype(
        jnp.bfloat16
    )
    pre_content = pre_both[:, :local_width].astype(jnp.float32)
    pre_gating = pre_both[:, local_width:].astype(jnp.float32)
    content = jax.nn.gelu(pre_content, approximate=False)
    gating = jax.nn.gelu(pre_gating, approximate=False)
    spatial, keeper = causal_table(mixing_weight)
    grad_wide = out_grad.astype(jnp.float32)
    mixed_grad = (grad_wide * content).astype(jnp.bfloat16)
    mixed_blocks = mixed_grad.reshape(blocks, BLOCK, groups_here, GROUP_DIM)
    normed_grad = jnp.einsum(
        "gts,btgc->bsgc", spatial, mixed_blocks, preferred_element_type=jnp.float32
    )
    centred_grad = normed_grad.reshape(tok_rows, local_width) * norm_gain[None, :]
    row_sum, row_square, grad_sum, grad_raw = lax.psum(
        (
            jnp.sum(gating, axis=1),
            jnp.sum(gating * gating, axis=1),
            jnp.sum(centred_grad, axis=1),
            jnp.sum(centred_grad * gating, axis=1),
        ),
        "dp",
    )
    row_mean = (row_sum / full_width)[:, None]
    row_var = (row_square / full_width)[:, None] - row_mean * row_mean
    inv_std = lax.rsqrt(row_var + norm_eps)
    centred = (gating - row_mean) * inv_std
    first_moment = (grad_sum / full_width)[:, None]
    second_moment = inv_std * ((grad_raw / full_width)[:, None] - row_mean * first_moment)
    normed = (centred * norm_gain[None, :]).astype(jnp.bfloat16)
    normed_blocks = normed.reshape(blocks, BLOCK, groups_here, GROUP_DIM)
    mixed = jnp.einsum("gts,bsgc->btgc", spatial, normed_blocks, preferred_element_type=jnp.float32)
    mixed = (mixed + jnp.transpose(mixing_bias)[None, :, :, None]).reshape(tok_rows, local_width)
    content_pre_grad = (grad_wide * mixed * gelu_slope(pre_content)).astype(jnp.bfloat16)
    local_mixing = jnp.einsum(
        "btgc,bsgc->gts", mixed_blocks, normed_blocks, preferred_element_type=jnp.float32
    )
    local_mixing = jnp.where(keeper, local_mixing, 0.0)
    mixing_grad = lax.psum(local_mixing.astype(jnp.bfloat16), "sp").astype(jnp.float32) * grad_scale
    gating_back = inv_std * (centred_grad - first_moment - centred * second_moment)
    gating_pre_grad = (gating_back * gelu_slope(pre_gating)).astype(jnp.bfloat16)
    joined_grad = jnp.concatenate([content_pre_grad, gating_pre_grad], axis=1)
    partial_input = lax.dot_general(
        joined_grad, joined_weight, (((1,), (1,)), ((), ())), preferred_element_type=jnp.float32
    )
    input_grad = lax.psum_scatter(
        partial_input.astype(jnp.bfloat16), "dp", scatter_dimension=1, tiled=True
    )
    both_grads = (
        lax.psum_scatter(
            hidden_term(hidden_in, joined_grad).astype(jnp.bfloat16),
            "sp",
            scatter_dimension=0,
            tiled=True,
        ).astype(jnp.float32)
        * grad_scale
    )
    content_grad = both_grads[:, :local_width]
    gating_grad = both_grads[:, local_width:]
    return (input_grad, content_grad, gating_grad, mixing_grad)


def phi_and_slope(values):
    cumulative = 0.5 * (1.0 + lax.erf(values * (1.0 / math.sqrt(2.0))))
    density = jnp.exp(-0.5 * values * values) * (1.0 / math.sqrt(2.0 * math.pi))
    return cumulative, cumulative + values * density


def dot(a, b, ca, cb):
    return lax.dot_general(
        a, b, (((ca,), (cb,)), ((), ())), preferred_element_type=jnp.float32
    )


def fused_kernel(
    n_dp, full_width, grad_scale,
    h_in, wc_in, wg_in, gain_in, mix_in, bias_in, og_in,
    x_out, c_out, g_out, m_out,
    gain_ref, mix_ref, bias_ref, hid, hid_t, wts, og, cg, cg_t, cs, gat, slope_g, mg, joined,
    stat_a, stat_quad, stat_b, stat_z,
    part, r_core, q_send, r_y, z_send, r_z, acc,
    gs, gr, go, ms, mr,
    load_sem, w_send, w_recv, sq_send, sq_recv, sz_send, sz_recv,
    core_send, core_recv, y_send, y_recv, zz_send, zz_recv,
    gx_send, gx_recv, mx_send, mx_recv,
):
    toks = hid.shape[0]
    chunks = toks // BLOCK
    shard = wc_in.shape[0]
    nz = n_dp // 4
    half = toks // 2
    tiles = gs.shape[0]
    tile = gs.shape[1]
    bf16 = jnp.bfloat16
    f32 = jnp.float32

    i = lax.axis_index("sp")
    j = lax.axis_index("dp")
    x_peer = 1 - i
    c = lax.rem(j, 2)
    y = lax.rem(j // 2, 2)
    z = j // 4
    j_core = j + 1 - 2 * c
    j_y = j + 2 - 4 * y
    j_diag = j_core + 2 - 4 * y

    mid = lax.rem((z + 1) // 2, 2)
    z_xor = (z, z + 1 - 2 * lax.rem(z, 2), z + 2 - 4 * (z // 2), 3 - z)

    def z_dev(q):
        return z_xor[q] * 4 + y * 2 + c

    def dev(a, b):
        return {"sp": a, "dp": b}

    def remote(src, dst, ssem, rsem, target):
        return pltpu.make_async_remote_copy(
            src_ref=src, dst_ref=dst, send_sem=ssem, recv_sem=rsem,
            device_id=target, device_id_type=pl.DeviceIdType.MESH,
        )

    mine = pl.multiple_of(i * shard, shard)
    theirs = pl.multiple_of(x_peer * shard, shard)
    loads = [
        pltpu.make_async_copy(wc_in, wts.at[pl.ds(mine, shard), pl.ds(0, BLOCK)], load_sem.at[0]),
        pltpu.make_async_copy(h_in, hid, load_sem.at[1]),
        pltpu.make_async_copy(wg_in, wts.at[pl.ds(mine, shard), pl.ds(BLOCK, BLOCK)], load_sem.at[2]),
        pltpu.make_async_copy(og_in, og, load_sem.at[3]),
        pltpu.make_async_copy(gain_in, gain_ref, load_sem.at[4]),
        pltpu.make_async_copy(mix_in, mix_ref, load_sem.at[5]),
        pltpu.make_async_copy(bias_in, bias_ref, load_sem.at[6]),
    ]
    for load in loads:
        load.start()

    barrier = pltpu.get_barrier_semaphore()
    peers = [dev(x_peer, j), dev(i, j_core), dev(i, j_y), dev(i, j_diag)]
    peers += [dev(i, z_dev(q)) for q in range(1, nz)]
    for peer in peers:
        pl.semaphore_signal(barrier, inc=1, device_id=peer, device_id_type=pl.DeviceIdType.MESH)
    pl.semaphore_wait(barrier, len(peers))

    pieces = w_send.shape[0] // 2
    piece = shard // pieces
    w_copies = []
    for which, src in ((0, wc_in), (1, wg_in)):
        for p in range(pieces):
            copy = remote(
                src.at[pl.ds(p * piece, piece), :],
                wts.at[pl.ds(pl.multiple_of(mine + p * piece, piece), piece), pl.ds(which * BLOCK, BLOCK)],
                w_send.at[which * pieces + p], w_recv.at[which * pieces + p],
                dev(x_peer, j),
            )
            copy.start()
            w_copies.append(copy)

    keep = lax.broadcasted_iota(jnp.int32, (BLOCK, BLOCK), 1) <= lax.broadcasted_iota(
        jnp.int32, (BLOCK, BLOCK), 0
    )
    for load in loads:
        load.wait()
    spatial = jnp.where(keep, mix_ref[0].astype(f32), 0.0).astype(bf16)
    gain = gain_ref[...]
    bias = jnp.broadcast_to(bias_ref[...], (BLOCK, BLOCK)).T
    own = dot(hid[:, pl.ds(mine, shard)], wts[pl.ds(mine, shard), :], 1, 0)
    joined_pre = own
    acc_c = go.at[pl.ds(0, toks), pl.ds(0, BLOCK)]
    acc_g = go.at[pl.ds(0, toks), pl.ds(BLOCK, BLOCK)]
    go[pl.ds(0, toks), :] = joined_pre
    for b in range(hid.shape[1] // BLOCK):
        hid_t[pl.ds(b * BLOCK, BLOCK), :] = hid[:, pl.ds(b * BLOCK, BLOCK)].T

    def finish(which, target):
        for p in range(pieces):
            w_copies[which * pieces + p].wait_recv()
            at = pl.multiple_of(theirs + p * piece, piece)
            target[...] += dot(
                hid[:, pl.ds(at, piece)], wts[pl.ds(at, piece), pl.ds(which * BLOCK, BLOCK)], 1, 0
            )

    finish(0, acc_c)
    for k in range(chunks):
        rows = pl.ds(k * BLOCK, BLOCK)
        pre = go[rows, 0:BLOCK].astype(bf16).astype(f32)
        wide = og[rows, :].astype(f32)
        cumulative, slope = phi_and_slope(pre)
        cs[rows, :] = wide * slope
        mixed_grad = (wide * (pre * cumulative)).astype(bf16)
        mg[rows, :] = mixed_grad
        centred_grad = dot(spatial, mixed_grad, 0, 0) * gain
        cg[rows, :] = centred_grad
        cg_t[rows, :] = centred_grad.T

    finish(1, acc_g)
    for k in range(chunks):
        rows = pl.ds(k * BLOCK, BLOCK)
        pre = go[rows, BLOCK:2 * BLOCK].astype(bf16).astype(f32)
        cumulative, slope = phi_and_slope(pre)
        gating = pre * cumulative
        gat[rows, :] = gating
        slope_g[rows, :] = slope
        turned = gating.T
        grad_turned = cg_t[rows, :]
        base = 4 * (k * BLOCK // half)
        cols = pl.ds(k * BLOCK % half, BLOCK)
        for row, table in enumerate((turned, turned * turned, grad_turned, grad_turned * turned)):
            stat_a[base + row:base + row + 1, cols] = jnp.sum(table, axis=0, keepdims=True)

    stat_copies = []
    for s, target in enumerate((j_core, j_y, j_diag)):
        copy = remote(stat_a, stat_quad.at[s], sq_send.at[s], sq_recv.at[s], dev(i, target))
        copy.start()
        stat_copies.append(copy)
    for copy in stat_copies:
        copy.wait()
    stat_b[...] = (stat_a[...] + stat_quad[0]) + (stat_quad[1] + stat_quad[2])
    stat_copies = []
    for q in range(1, nz):
        copy = remote(
            stat_b, stat_z.at[q - 1], sz_send.at[q - 1], sz_recv.at[q - 1], dev(i, z_dev(q))
        )
        copy.start()
        stat_copies.append(copy)
    for copy in stat_copies:
        copy.wait()
    total = stat_b[...]
    for q in range(1, nz):
        total = total + stat_z[q - 1]
    total = total * (1.0 / full_width)

    mixing = jnp.zeros((BLOCK, BLOCK), f32)
    for k in range(chunks):
        rows = pl.ds(k * BLOCK, BLOCK)
        base = 4 * (k * BLOCK // half)
        col = k * BLOCK % half
        part_of = total[base:base + 4, col:col + BLOCK]
        mean = part_of[0:1]
        inv = lax.rsqrt(part_of[1:2] - mean * mean + norm_eps)
        first = part_of[2:3]
        second = inv * (part_of[3:4] - mean * first)

        def spread(row):
            return jnp.broadcast_to(row, (BLOCK, BLOCK)).T

        inv_w = spread(inv)
        centred = (gat[rows, :] - spread(mean)) * inv_w
        normed = (centred * gain).astype(bf16)
        mixed = dot(spatial, normed, 1, 0) + bias
        joined[rows, 0:BLOCK] = (cs[rows, :] * mixed).astype(bf16)
        back = inv_w * (cg[rows, :] - spread(first) - centred * spread(second))
        joined[rows, BLOCK:2 * BLOCK] = (back * slope_g[rows, :]).astype(bf16)
        mixing = mixing + dot(mg[rows, :], normed, 1, 1)
    mixing = jnp.where(keep, mixing, 0.0)

    waits = []
    order = [(slot, h) for slot in range(nz) for h in range(2)]
    pieces_in = len(order)

    def input_part(n):
        slot, h = order[n]
        grads = joined[pl.ds(h * half, half), :]
        at = pl.multiple_of(z_xor[3 - slot] * (4 * BLOCK), 4 * BLOCK)
        res = dot(grads, wts[pl.ds(at, 4 * BLOCK), :], 1, 1).astype(bf16)
        for yy in range(2):
            for cc in range(2):
                at = (yy * 2 + cc) * BLOCK
                part[n, cc, yy] = res[:, at:at + BLOCK]
        copy = remote(part.at[n, 1 - c], r_core.at[n], core_send.at[n], core_recv.at[n], dev(i, j_core))
        copy.start()
        waits.append(copy)
        core_copies[n] = copy

    def weight_part(t):
        at = pl.multiple_of(theirs + t * tile, tile)
        gs[t] = dot(hid_t[pl.ds(at, tile), :], joined[...], 1, 0).astype(bf16)
        copy = remote(gs.at[t], gr.at[t], gx_send.at[t], gx_recv.at[t], dev(x_peer, j))
        copy.start()
        waits.append(copy)
        return copy

    core_copies, y_copies, z_copies, g_copies = {}, {}, {}, {}

    def second_stage(n):
        core_copies[n].wait_recv()
        q_send[n] = (part[n, c, 1 - y].astype(f32) + r_core[n, 1 - y].astype(f32)).astype(bf16)
        copy = remote(q_send.at[n], r_y.at[n], y_send.at[n], y_recv.at[n], dev(i, j_y))
        copy.start()
        waits.append(copy)
        y_copies[n] = copy

    def direct(h):
        return remote(z_send.at[0, h], r_z.at[0, h], zz_send.at[0, h], zz_recv.at[0, h], dev(i, z_dev(3)))

    def relay(h):
        return remote(z_send.at[0, h], r_z.at[3, h], zz_send.at[0, h], zz_recv.at[3, h], dev(i, z_dev(1)))

    def third_stage(n):
        slot, h = order[n]
        y_copies[n].wait_recv()
        res = (part[n, c, y].astype(f32) + r_core[n, y].astype(f32)) + r_y[n].astype(f32)
        if slot == nz - 1:
            acc[h] = res
            return
        if slot == 0:
            z_send[0, h] = res.astype(bf16)

            @pl.when(mid == 1)
            def _():
                direct(h).start()

            @pl.when(mid == 0)
            def _():
                relay(h).start()

            waits.append(direct(h))
            return
        if slot == 1:

            @pl.when(mid == 1)
            def _():
                relay(h).wait_recv()
                z_send[1, h] = (res + r_z[3, h].astype(f32)).astype(bf16)

            @pl.when(mid == 0)
            def _():
                z_send[1, h] = res.astype(bf16)
        else:
            z_send[slot, h] = res.astype(bf16)
        copy = remote(
            z_send.at[slot, h], r_z.at[slot, h], zz_send.at[slot, h], zz_recv.at[slot, h], dev(i, z_dev(3 - slot))
        )
        copy.start()
        waits.append(copy)
        z_copies[slot, h] = copy

    def last_stage(h):
        @pl.when(mid == 1)
        def _():
            direct(h).wait_recv()
            acc[h] = acc[h] + r_z[0, h].astype(f32)

        res = acc[h]
        for slot in range(1, nz - 1):
            z_copies[slot, h].wait_recv()
            res = res + r_z[slot, h].astype(f32)
        x_out[pl.ds(h * half, half), :] = res.astype(bf16)

    for step in range(pieces_in + 2):
        if step < pieces_in:
            input_part(step)
        if step < tiles:
            g_copies[step] = weight_part(step)
        if step >= 2:
            second_stage(step - 2)
    ms[...] = mixing.astype(bf16)
    m_copy = remote(ms, mr, mx_send, mx_recv, dev(x_peer, j))
    m_copy.start()
    waits.append(m_copy)
    for t in range(tiles):
        at = pl.multiple_of(mine + t * tile, tile)
        go[pl.ds(t * tile, tile), :] = dot(hid_t[pl.ds(at, tile), :], joined[...], 1, 0)
    for n in range(pieces_in):
        third_stage(n)
    for h in range(2):
        last_stage(h)
    for t in range(tiles):
        g_copies[t].wait_recv()
        rows = pl.ds(t * tile, tile)
        res = (go[rows, :] + gr[t].astype(f32)) * grad_scale
        c_out[rows, :] = res[:, 0:BLOCK]
        g_out[rows, :] = res[:, BLOCK:2 * BLOCK]
    m_copy.wait_recv()
    m_out[0] = (mixing + mr[...].astype(f32)) * grad_scale
    for copy in w_copies + waits:
        copy.wait_send()


def fused(n_dp, hidden_in, content_weight, gating_weight, norm_gain, mixing_weight, mixing_bias, out_grad):
    toks, depth = hidden_in.shape
    shard, width = content_weight.shape
    half = toks // 2
    nz = n_dp // 4
    tile = 256
    tiles = shard // tile
    pieces = 2
    grad_scale = 1.0 / math.sqrt(2 * toks)
    bf16, f32 = jnp.bfloat16, jnp.float32
    vmem = pl.BlockSpec(memory_space=pltpu.VMEM)
    anywhere = pl.BlockSpec(memory_space=pl.ANY)
    dma = pltpu.SemaphoreType.DMA
    V = pltpu.VMEM
    scratch = [
        V((1, width), f32), V((1, BLOCK, BLOCK), bf16), V((1, BLOCK), f32),
        V((toks, depth), bf16), V((depth, toks), bf16), V((depth, 2 * width), bf16), V((toks, width), bf16),
        V((toks, width), f32), V((toks, width), f32), V((toks, width), f32), V((toks, width), f32),
        V((toks, width), f32), V((toks, width), bf16), V((toks, 2 * width), bf16),
        V((8, toks // 2), f32), V((3, 8, toks // 2), f32), V((8, toks // 2), f32), V((nz - 1, 8, toks // 2), f32),
        V((2 * nz, 2, 2, half, width), bf16), V((2 * nz, 2, half, width), bf16),
        V((2 * nz, half, width), bf16), V((2 * nz, half, width), bf16),
        V((nz - 1, 2, half, width), bf16), V((nz, 2, half, width), bf16), V((2, half, width), f32),
        V((tiles, tile, 2 * width), bf16), V((tiles, tile, 2 * width), bf16), V((shard, 2 * width), f32),
        V((BLOCK, BLOCK), bf16), V((BLOCK, BLOCK), bf16),
        dma((7,)), dma((2 * pieces,)), dma((2 * pieces,)), dma((3,)), dma((3,)), dma((nz - 1,)), dma((nz - 1,)),
        dma((2 * nz,)), dma((2 * nz,)), dma((2 * nz,)), dma((2 * nz,)), dma((nz - 1, 2)), dma((nz, 2)),
        dma((tiles,)), dma((tiles,)), dma, dma,
    ]
    return pl.pallas_call(
        functools.partial(fused_kernel, n_dp, width * n_dp, grad_scale),
        out_shape=(
            jax.ShapeDtypeStruct((toks, width), bf16),
            jax.ShapeDtypeStruct((shard, width), f32),
            jax.ShapeDtypeStruct((shard, width), f32),
            jax.ShapeDtypeStruct(mixing_weight.shape, f32),
        ),
        in_specs=[anywhere] * 7,
        out_specs=(vmem,) * 4,
        scratch_shapes=scratch,
        compiler_params=pltpu.CompilerParams(
            collective_id=0, has_side_effects=True, vmem_limit_bytes=67043328
        ),
    )(hidden_in, content_weight, gating_weight, norm_gain[None, :], mixing_weight, mixing_bias, out_grad)


def fits(n_sp, n_dp, toks, shard, width):
    paired = n_sp == 2 and n_dp == 16
    return paired and width == GROUP_DIM and shard % 512 == 0 and toks % (2 * BLOCK) == 0 and toks <= shard


def solve(*args):
    n_sp, n_dp = lax.axis_size("sp"), lax.axis_size("dp")
    shard, width = args[1].shape
    if fits(n_sp, n_dp, args[0].shape[0], shard, width) and args[0].shape[1] == n_dp * width:
        return fused(n_dp, *args)
    return local(*args)


def solution(mesh):
    in_specs = (
        P("sp", None),
        P("sp", "dp"),
        P("sp", "dp"),
        P("dp"),
        P("dp", None, None),
        P("dp", None),
        P("sp", "dp"),
    )
    out_specs = (P("sp", "dp"), P("sp", "dp"), P("sp", "dp"), P("dp", None, None))
    return jax.shard_map(solve, mesh=mesh, in_specs=in_specs, out_specs=out_specs, check_vma=False)
```

```python
import functools
import math

import jax
import jax.numpy as jnp
from jax import lax
from jax.experimental import pallas as pl
from jax.experimental.pallas import tpu as pltpu
from jax.sharding import PartitionSpec as P

GROUP_DIM = 128
BLOCK = 128


norm_eps = 1e-05


def gelu_slope(values):
    cumulative = 0.5 * (1.0 + lax.erf(values * (1.0 / math.sqrt(2.0))))
    density = jnp.exp(-0.5 * values * values) * (1.0 / math.sqrt(2.0 * math.pi))
    return cumulative + values * density


def causal_table(weights):
    row_ids = lax.broadcasted_iota(jnp.int32, (BLOCK, BLOCK), 0)
    col_ids = lax.broadcasted_iota(jnp.int32, (BLOCK, BLOCK), 1)
    keeper = (col_ids <= row_ids)[None]
    return (jnp.where(keeper, weights, jnp.zeros_like(weights)), keeper)


def hidden_term(hidden_in, grads):
    return lax.dot_general(
        hidden_in, grads, (((0,), (0,)), ((), ())), preferred_element_type=jnp.float32
    )


def local(
    hidden_in, content_weight, gating_weight, norm_gain, mixing_weight, mixing_bias, out_grad
):
    tok_rows = hidden_in.shape[0]
    local_width = content_weight.shape[1]
    groups_here = local_width // GROUP_DIM
    blocks = tok_rows // BLOCK
    full_width = local_width * lax.axis_size("dp")
    grad_scale = 1.0 / math.sqrt(tok_rows * lax.axis_size("sp"))
    whole_content, whole_gating = (
        lax.all_gather(content_weight, "sp", axis=0, tiled=True),
        lax.all_gather(gating_weight, "sp", axis=0, tiled=True),
    )
    joined_weight = jnp.concatenate([whole_content, whole_gating], axis=1)
    pre_both = jnp.dot(hidden_in, joined_weight, preferred_element_type=jnp.float32).astype(
        jnp.bfloat16
    )
    pre_content = pre_both[:, :local_width].astype(jnp.float32)
    pre_gating = pre_both[:, local_width:].astype(jnp.float32)
    content = jax.nn.gelu(pre_content, approximate=False)
    gating = jax.nn.gelu(pre_gating, approximate=False)
    spatial, keeper = causal_table(mixing_weight)
    grad_wide = out_grad.astype(jnp.float32)
    mixed_grad = (grad_wide * content).astype(jnp.bfloat16)
    mixed_blocks = mixed_grad.reshape(blocks, BLOCK, groups_here, GROUP_DIM)
    normed_grad = jnp.einsum(
        "gts,btgc->bsgc", spatial, mixed_blocks, preferred_element_type=jnp.float32
    )
    centred_grad = normed_grad.reshape(tok_rows, local_width) * norm_gain[None, :]
    row_sum, row_square, grad_sum, grad_raw = lax.psum(
        (
            jnp.sum(gating, axis=1),
            jnp.sum(gating * gating, axis=1),
            jnp.sum(centred_grad, axis=1),
            jnp.sum(centred_grad * gating, axis=1),
        ),
        "dp",
    )
    row_mean = (row_sum / full_width)[:, None]
    row_var = (row_square / full_width)[:, None] - row_mean * row_mean
    inv_std = lax.rsqrt(row_var + norm_eps)
    centred = (gating - row_mean) * inv_std
    first_moment = (grad_sum / full_width)[:, None]
    second_moment = inv_std * ((grad_raw / full_width)[:, None] - row_mean * first_moment)
    normed = (centred * norm_gain[None, :]).astype(jnp.bfloat16)
    normed_blocks = normed.reshape(blocks, BLOCK, groups_here, GROUP_DIM)
    mixed = jnp.einsum("gts,bsgc->btgc", spatial, normed_blocks, preferred_element_type=jnp.float32)
    mixed = (mixed + jnp.transpose(mixing_bias)[None, :, :, None]).reshape(tok_rows, local_width)
    content_pre_grad = (grad_wide * mixed * gelu_slope(pre_content)).astype(jnp.bfloat16)
    local_mixing = jnp.einsum(
        "btgc,bsgc->gts", mixed_blocks, normed_blocks, preferred_element_type=jnp.float32
    )
    local_mixing = jnp.where(keeper, local_mixing, 0.0)
    mixing_grad = lax.psum(local_mixing.astype(jnp.bfloat16), "sp").astype(jnp.float32) * grad_scale
    gating_back = inv_std * (centred_grad - first_moment - centred * second_moment)
    gating_pre_grad = (gating_back * gelu_slope(pre_gating)).astype(jnp.bfloat16)
    joined_grad = jnp.concatenate([content_pre_grad, gating_pre_grad], axis=1)
    partial_input = lax.dot_general(
        joined_grad, joined_weight, (((1,), (1,)), ((), ())), preferred_element_type=jnp.float32
    )
    input_grad = lax.psum_scatter(
        partial_input.astype(jnp.bfloat16), "dp", scatter_dimension=1, tiled=True
    )
    both_grads = (
        lax.psum_scatter(
            hidden_term(hidden_in, joined_grad).astype(jnp.bfloat16),
            "sp",
            scatter_dimension=0,
            tiled=True,
        ).astype(jnp.float32)
        * grad_scale
    )
    content_grad = both_grads[:, :local_width]
    gating_grad = both_grads[:, local_width:]
    return (input_grad, content_grad, gating_grad, mixing_grad)


def phi_and_slope(values):
    cumulative = 0.5 * (1.0 + lax.erf(values * (1.0 / math.sqrt(2.0))))
    density = jnp.exp(-0.5 * values * values) * (1.0 / math.sqrt(2.0 * math.pi))
    return cumulative, cumulative + values * density


def dot(a, b, ca, cb):
    return lax.dot_general(
        a, b, (((ca,), (cb,)), ((), ())), preferred_element_type=jnp.float32
    )


def fused_kernel(
    n_dp, full_width, grad_scale,
    h_in, wc_in, wg_in, gain_in, mix_in, bias_in, og_in,
    x_out, c_out, g_out, m_out,
    gain_ref, mix_ref, bias_ref, hid, hid_t, wts, og, cg, cg_t, cs, gat, slope_g, mg, joined,
    stat_a, stat_quad, stat_b, stat_z,
    part, r_core, q_send, r_y, z_send, r_z, acc,
    gs, gr, go, ms, mr,
    load_sem, w_send, w_recv, sq_send, sq_recv, sz_send, sz_recv,
    core_send, core_recv, y_send, y_recv, zz_send, zz_recv,
    gx_send, gx_recv, mx_send, mx_recv, out_sem, x_buf, m_buf,
):
    toks = hid.shape[0]
    chunks = toks // BLOCK
    shard = wc_in.shape[0]
    nz = n_dp // 4
    half = toks // 2
    tiles = gs.shape[0]
    tile = gs.shape[1]
    bf16 = jnp.bfloat16
    f32 = jnp.float32

    i = lax.axis_index("sp")
    j = lax.axis_index("dp")
    x_peer = 1 - i
    c = lax.rem(j, 2)
    y = lax.rem(j // 2, 2)
    z = j // 4
    j_core = j + 1 - 2 * c
    j_y = j + 2 - 4 * y
    j_diag = j_core + 2 - 4 * y

    mid = lax.rem((z + 1) // 2, 2)
    z_xor = (z, z + 1 - 2 * lax.rem(z, 2), z + 2 - 4 * (z // 2), 3 - z)

    def z_dev(q):
        return z_xor[q] * 4 + y * 2 + c

    def dev(a, b):
        return {"sp": a, "dp": b}

    def remote(src, dst, ssem, rsem, target):
        return pltpu.make_async_remote_copy(
            src_ref=src, dst_ref=dst, send_sem=ssem, recv_sem=rsem,
            device_id=target, device_id_type=pl.DeviceIdType.MESH,
        )

    mine = pl.multiple_of(i * shard, shard)
    theirs = pl.multiple_of(x_peer * shard, shard)
    loads = [
        pltpu.make_async_copy(wc_in, wts.at[pl.ds(mine, shard), pl.ds(0, BLOCK)], load_sem.at[0]),
        pltpu.make_async_copy(h_in, hid, load_sem.at[1]),
        pltpu.make_async_copy(wg_in, wts.at[pl.ds(mine, shard), pl.ds(BLOCK, BLOCK)], load_sem.at[2]),
        pltpu.make_async_copy(og_in, og, load_sem.at[3]),
        pltpu.make_async_copy(gain_in, gain_ref, load_sem.at[4]),
        pltpu.make_async_copy(mix_in, mix_ref, load_sem.at[5]),
        pltpu.make_async_copy(bias_in, bias_ref, load_sem.at[6]),
    ]
    for load in loads:
        load.start()

    barrier = pltpu.get_barrier_semaphore()
    peers = [dev(x_peer, j), dev(i, j_core), dev(i, j_y), dev(i, j_diag)]
    peers += [dev(i, z_dev(q)) for q in range(1, nz)]
    for peer in peers:
        pl.semaphore_signal(barrier, inc=1, device_id=peer, device_id_type=pl.DeviceIdType.MESH)
    pl.semaphore_wait(barrier, len(peers))

    pieces = w_send.shape[0] // 2
    piece = shard // pieces
    w_copies = []
    for which, src in ((0, wc_in), (1, wg_in)):
        for p in range(pieces):
            copy = remote(
                src.at[pl.ds(p * piece, piece), :],
                wts.at[pl.ds(pl.multiple_of(mine + p * piece, piece), piece), pl.ds(which * BLOCK, BLOCK)],
                w_send.at[which * pieces + p], w_recv.at[which * pieces + p],
                dev(x_peer, j),
            )
            copy.start()
            w_copies.append(copy)

    keep = lax.broadcasted_iota(jnp.int32, (BLOCK, BLOCK), 1) <= lax.broadcasted_iota(
        jnp.int32, (BLOCK, BLOCK), 0
    )
    for load in loads:
        load.wait()
    spatial = jnp.where(keep, mix_ref[0].astype(f32), 0.0).astype(bf16)
    gain = gain_ref[...]
    bias = jnp.broadcast_to(bias_ref[...], (BLOCK, BLOCK)).T
    own = dot(hid[:, pl.ds(mine, shard)], wts[pl.ds(mine, shard), :], 1, 0)
    joined_pre = own
    acc_c = go.at[pl.ds(0, toks), pl.ds(0, BLOCK)]
    acc_g = go.at[pl.ds(0, toks), pl.ds(BLOCK, BLOCK)]
    go[pl.ds(0, toks), :] = joined_pre
    for b in range(hid.shape[1] // BLOCK):
        hid_t[pl.ds(b * BLOCK, BLOCK), :] = hid[:, pl.ds(b * BLOCK, BLOCK)].T

    def finish(which, target):
        for p in range(pieces):
            w_copies[which * pieces + p].wait_recv()
            at = pl.multiple_of(theirs + p * piece, piece)
            target[...] += dot(
                hid[:, pl.ds(at, piece)], wts[pl.ds(at, piece), pl.ds(which * BLOCK, BLOCK)], 1, 0
            )

    finish(0, acc_c)
    for k in range(chunks):
        rows = pl.ds(k * BLOCK, BLOCK)
        pre = go[rows, 0:BLOCK].astype(bf16).astype(f32)
        wide = og[rows, :].astype(f32)
        cumulative, slope = phi_and_slope(pre)
        cs[rows, :] = wide * slope
        mixed_grad = (wide * (pre * cumulative)).astype(bf16)
        mg[rows, :] = mixed_grad
        centred_grad = dot(spatial, mixed_grad, 0, 0) * gain
        cg[rows, :] = centred_grad
        cg_t[rows, :] = centred_grad.T

    finish(1, acc_g)
    for k in range(chunks):
        rows = pl.ds(k * BLOCK, BLOCK)
        pre = go[rows, BLOCK:2 * BLOCK].astype(bf16).astype(f32)
        cumulative, slope = phi_and_slope(pre)
        gating = pre * cumulative
        gat[rows, :] = gating
        slope_g[rows, :] = slope
        turned = gating.T
        grad_turned = cg_t[rows, :]
        base = 4 * (k * BLOCK // half)
        cols = pl.ds(k * BLOCK % half, BLOCK)
        for row, table in enumerate((turned, turned * turned, grad_turned, grad_turned * turned)):
            stat_a[base + row:base + row + 1, cols] = jnp.sum(table, axis=0, keepdims=True)

    stat_copies = []
    for s, target in enumerate((j_core, j_y, j_diag)):
        copy = remote(stat_a, stat_quad.at[s], sq_send.at[s], sq_recv.at[s], dev(i, target))
        copy.start()
        stat_copies.append(copy)
    for copy in stat_copies:
        copy.wait()
    stat_b[...] = (stat_a[...] + stat_quad[0]) + (stat_quad[1] + stat_quad[2])
    stat_copies = []
    for q in range(1, nz):
        copy = remote(
            stat_b, stat_z.at[q - 1], sz_send.at[q - 1], sz_recv.at[q - 1], dev(i, z_dev(q))
        )
        copy.start()
        stat_copies.append(copy)
    for copy in stat_copies:
        copy.wait()
    total = stat_b[...]
    for q in range(1, nz):
        total = total + stat_z[q - 1]
    total = total * (1.0 / full_width)

    mixing = jnp.zeros((BLOCK, BLOCK), f32)
    for k in range(chunks):
        rows = pl.ds(k * BLOCK, BLOCK)
        base = 4 * (k * BLOCK // half)
        col = k * BLOCK % half
        part_of = total[base:base + 4, col:col + BLOCK]
        mean = part_of[0:1]
        inv = lax.rsqrt(part_of[1:2] - mean * mean + norm_eps)
        first = part_of[2:3]
        second = inv * (part_of[3:4] - mean * first)

        def spread(row):
            return jnp.broadcast_to(row, (BLOCK, BLOCK)).T

        inv_w = spread(inv)
        centred = (gat[rows, :] - spread(mean)) * inv_w
        normed = (centred * gain).astype(bf16)
        mixed = dot(spatial, normed, 1, 0) + bias
        joined[rows, 0:BLOCK] = (cs[rows, :] * mixed).astype(bf16)
        back = inv_w * (cg[rows, :] - spread(first) - centred * spread(second))
        joined[rows, BLOCK:2 * BLOCK] = (back * slope_g[rows, :]).astype(bf16)
        mixing = mixing + dot(mg[rows, :], normed, 1, 1)
    mixing = jnp.where(keep, mixing, 0.0)

    waits = []
    stores = []

    def store(src, dst):
        copy = pltpu.make_async_copy(src, dst, out_sem.at[len(stores)])
        copy.start()
        stores.append(copy)

    order = [(slot, h) for slot in range(nz) for h in range(2)]
    pieces_in = len(order)

    def input_part(n):
        slot, h = order[n]
        grads = joined[pl.ds(h * half, half), :]
        at = pl.multiple_of(z_xor[3 - slot] * (4 * BLOCK), 4 * BLOCK)
        res = dot(grads, wts[pl.ds(at, 4 * BLOCK), :], 1, 1).astype(bf16)
        for yy in range(2):
            for cc in range(2):
                at = (yy * 2 + cc) * BLOCK
                part[n, cc, yy] = res[:, at:at + BLOCK]
        copy = remote(part.at[n, 1 - c], r_core.at[n], core_send.at[n], core_recv.at[n], dev(i, j_core))
        copy.start()
        waits.append(copy)
        core_copies[n] = copy

    def weight_part(t):
        at = pl.multiple_of(theirs + t * tile, tile)
        gs[t] = dot(hid_t[pl.ds(at, tile), :], joined[...], 1, 0).astype(bf16)
        copy = remote(gs.at[t], gr.at[t], gx_send.at[t], gx_recv.at[t], dev(x_peer, j))
        copy.start()
        waits.append(copy)
        return copy

    core_copies, y_copies, z_copies, g_copies = {}, {}, {}, {}

    def second_stage(n):
        core_copies[n].wait_recv()
        q_send[n] = (part[n, c, 1 - y].astype(f32) + r_core[n, 1 - y].astype(f32)).astype(bf16)
        copy = remote(q_send.at[n], r_y.at[n], y_send.at[n], y_recv.at[n], dev(i, j_y))
        copy.start()
        waits.append(copy)
        y_copies[n] = copy

    def direct(h):
        return remote(z_send.at[0, h], r_z.at[0, h], zz_send.at[0, h], zz_recv.at[0, h], dev(i, z_dev(3)))

    def relay(h):
        return remote(z_send.at[0, h], r_z.at[3, h], zz_send.at[0, h], zz_recv.at[3, h], dev(i, z_dev(1)))

    def third_stage(n):
        slot, h = order[n]
        y_copies[n].wait_recv()
        res = (part[n, c, y].astype(f32) + r_core[n, y].astype(f32)) + r_y[n].astype(f32)
        if slot == nz - 1:
            acc[h] = res
            return
        if slot == 0:
            z_send[0, h] = res.astype(bf16)

            @pl.when(mid == 1)
            def _():
                direct(h).start()

            @pl.when(mid == 0)
            def _():
                relay(h).start()

            waits.append(direct(h))
            return
        if slot == 1:

            @pl.when(mid == 1)
            def _():
                relay(h).wait_recv()
                z_send[1, h] = (res + r_z[3, h].astype(f32)).astype(bf16)

            @pl.when(mid == 0)
            def _():
                z_send[1, h] = res.astype(bf16)
        else:
            z_send[slot, h] = res.astype(bf16)
        copy = remote(
            z_send.at[slot, h], r_z.at[slot, h], zz_send.at[slot, h], zz_recv.at[slot, h], dev(i, z_dev(3 - slot))
        )
        copy.start()
        waits.append(copy)
        z_copies[slot, h] = copy

    def last_stage(h):
        @pl.when(mid == 1)
        def _():
            direct(h).wait_recv()
            acc[h] = acc[h] + r_z[0, h].astype(f32)

        res = acc[h]
        for slot in range(1, nz - 1):
            z_copies[slot, h].wait_recv()
            res = res + r_z[slot, h].astype(f32)
        x_buf[pl.ds(h * half, half), :] = res.astype(bf16)
        store(x_buf.at[pl.ds(h * half, half), :], x_out.at[pl.ds(h * half, half), :])

    for step in range(pieces_in + 2):
        if step < pieces_in:
            input_part(step)
        if step < tiles:
            g_copies[step] = weight_part(step)
        if step >= 2:
            second_stage(step - 2)
    ms[...] = mixing.astype(bf16)
    m_copy = remote(ms, mr, mx_send, mx_recv, dev(x_peer, j))
    m_copy.start()
    waits.append(m_copy)
    for t in range(tiles):
        at = pl.multiple_of(mine + t * tile, tile)
        go[pl.ds(t * tile, tile), :] = dot(hid_t[pl.ds(at, tile), :], joined[...], 1, 0)
    for n in range(pieces_in):
        third_stage(n)
    for t in range(tiles):
        g_copies[t].wait_recv()
        rows = pl.ds(t * tile, tile)
        go[rows, :] = (go[rows, :] + gr[t].astype(f32)) * grad_scale
        store(go.at[rows, pl.ds(0, BLOCK)], c_out.at[rows, :])
        store(go.at[rows, pl.ds(BLOCK, BLOCK)], g_out.at[rows, :])
    m_copy.wait_recv()
    m_buf[0] = (mixing + mr[...].astype(f32)) * grad_scale
    store(m_buf, m_out)
    for h in range(2):
        last_stage(h)
    for copy in stores:
        copy.wait()
    for copy in w_copies + waits:
        copy.wait_send()


def store_kernel(*refs):
    count = len(refs) // 3
    src, dst, held = refs[:count], refs[count:2 * count], refs[2 * count:3 * count]
    sem = refs[-1]
    loads = [pltpu.make_async_copy(src[k], held[k], sem.at[0, k]) for k in range(count)]
    stores = [pltpu.make_async_copy(held[k], dst[k], sem.at[1, k]) for k in range(count)]
    for load in loads:
        load.start()
    for load, store in zip(loads, stores):
        load.wait()
        store.start()
    for store in stores:
        store.wait()


def fused(n_dp, hidden_in, content_weight, gating_weight, norm_gain, mixing_weight, mixing_bias, out_grad):
    toks, depth = hidden_in.shape
    shard, width = content_weight.shape
    half = toks // 2
    nz = n_dp // 4
    tile = 256
    tiles = shard // tile
    pieces = 2
    grad_scale = 1.0 / math.sqrt(2 * toks)
    bf16, f32 = jnp.bfloat16, jnp.float32
    in_hbm = pl.BlockSpec(memory_space=pltpu.HBM)
    dma = pltpu.SemaphoreType.DMA
    V = pltpu.VMEM
    scratch = [
        V((1, width), f32), V((1, BLOCK, BLOCK), bf16), V((1, BLOCK), f32),
        V((toks, depth), bf16), V((depth, toks), bf16), V((depth, 2 * width), bf16), V((toks, width), bf16),
        V((toks, width), f32), V((toks, width), f32), V((toks, width), f32), V((toks, width), f32),
        V((toks, width), f32), V((toks, width), bf16), V((toks, 2 * width), bf16),
        V((8, toks // 2), f32), V((3, 8, toks // 2), f32), V((8, toks // 2), f32), V((nz - 1, 8, toks // 2), f32),
        V((2 * nz, 2, 2, half, width), bf16), V((2 * nz, 2, half, width), bf16),
        V((2 * nz, half, width), bf16), V((2 * nz, half, width), bf16),
        V((nz - 1, 2, half, width), bf16), V((nz, 2, half, width), bf16), V((2, half, width), f32),
        V((tiles, tile, 2 * width), bf16), V((tiles, tile, 2 * width), bf16), V((shard, 2 * width), f32),
        V((BLOCK, BLOCK), bf16), V((BLOCK, BLOCK), bf16),
        dma((7,)), dma((2 * pieces,)), dma((2 * pieces,)), dma((3,)), dma((3,)), dma((nz - 1,)), dma((nz - 1,)),
        dma((2 * nz,)), dma((2 * nz,)), dma((2 * nz,)), dma((2 * nz,)), dma((nz - 1, 2)), dma((nz, 2)),
        dma((tiles,)), dma((tiles,)), dma, dma, dma((2 * tiles + 3,)),
        V((toks, width), bf16), V((1, BLOCK, BLOCK), f32),
    ]
    results = pl.pallas_call(
        functools.partial(fused_kernel, n_dp, width * n_dp, grad_scale),
        out_shape=(
            jax.ShapeDtypeStruct((toks, width), bf16),
            jax.ShapeDtypeStruct((shard, width), f32),
            jax.ShapeDtypeStruct((shard, width), f32),
            jax.ShapeDtypeStruct(mixing_weight.shape, f32),
        ),
        in_specs=[in_hbm] * 7,
        out_specs=(in_hbm,) * 4,
        scratch_shapes=scratch,
        compiler_params=pltpu.CompilerParams(
            collective_id=0, has_side_effects=True, vmem_limit_bytes=67043328
        ),
    )(hidden_in, content_weight, gating_weight, norm_gain[None, :], mixing_weight, mixing_bias, out_grad)
    return pl.pallas_call(
        store_kernel,
        out_shape=tuple(jax.ShapeDtypeStruct(r.shape, r.dtype) for r in results),
        in_specs=[in_hbm] * 4,
        out_specs=(in_hbm,) * 4,
        scratch_shapes=[V(r.shape, r.dtype) for r in results] + [dma((2, 4))],
        compiler_params=pltpu.CompilerParams(vmem_limit_bytes=67043328),
    )(*results)


def fits(n_sp, n_dp, toks, shard, width):
    paired = n_sp == 2 and n_dp == 16
    return paired and width == GROUP_DIM and shard % 512 == 0 and toks % (2 * BLOCK) == 0 and toks <= shard


def solve(*args):
    n_sp, n_dp = lax.axis_size("sp"), lax.axis_size("dp")
    shard, width = args[1].shape
    if fits(n_sp, n_dp, args[0].shape[0], shard, width) and args[0].shape[1] == n_dp * width:
        return fused(n_dp, *args)
    return local(*args)


def solution(mesh):
    in_specs = (
        P("sp", None),
        P("sp", "dp"),
        P("sp", "dp"),
        P("dp"),
        P("dp", None, None),
        P("dp", None),
        P("sp", "dp"),
    )
    out_specs = (P("sp", "dp"), P("sp", "dp"), P("sp", "dp"), P("dp", None, None))
    return jax.shard_map(solve, mesh=mesh, in_specs=in_specs, out_specs=out_specs, check_vma=False)
```
